32 devices in a mesh: grp: 2 (over y), sp: 4 (over z), fs: 2 (over x), tp: 2 (over core).
Axes of the slice: x: 2, y: 2, z: 4, core: 2. Of those that a mesh axis runs over, the one named last changes fastest.
Arguments:
- tokens: bfloat16 [4, 1024, 2048], P(('grp', 'fs'), 'sp', 'tp'), parts along dimension 0, may hold values from -6 to 6
- input_norm_gain: float32 [2048], replicated, may hold values from 0.1 to 1.9
- query_weight: bfloat16 [2048, 1024], P('sp', 'tp'), may hold values from -0.125 to 0.125
- key_weight: bfloat16 [2048, 1024], P('sp', 'tp'), may hold values from -0.125 to 0.125
- value_weight: bfloat16 [2048, 1024], P('sp', 'tp'), may hold values from -0.125 to 0.125
- decay_gate_weight: bfloat16 [2048, 8], replicated, may hold values from -0.125 to 0.125
- write_strength_weight: bfloat16 [2048, 8], replicated, may hold values from -0.125 to 0.125
- up_weight: bfloat16 [2048, 1024], P('sp', 'tp'), may hold values from -0.125 to 0.125
- gate_half_weight: bfloat16 [2048, 1024], P('sp', 'tp'), may hold values from -0.125 to 0.125
- log_decay_rate: float32 [8], replicated, may hold values from -30 to 0
- write_strength_bias: float32 [8], replicated, may hold values from -7 to 1
- decay_spike_added: float32 [4, 1024, 8], P(('grp', 'fs'), 'sp', 'tp'), parts along dimension 0, may hold values from -2 to 0
- starting_state: float32 [4, 8, 128, 128], P(('grp', 'fs'), 'tp'), parts along dimension 0, may hold values from -4 to 4
- head_norm_gain: float32 [128], replicated, may hold values from 0.1 to 1.9
- convolution_kernel: float32 [31, 1024], replicated, may hold values from -4 to 4
- channel_norm_gain: float32 [1024], replicated, may hold values from 0.1 to 1.9
- delta_output_rows: bfloat16 [1024, 2048], P('tp', 'sp'), may hold values from -0.125 to 0.125
- convolution_output_rows: bfloat16 [1024, 2048], P('tp', 'sp'), may hold values from -0.125 to 0.125
Outputs:
- mixed: bfloat16 [4, 1024, 2048], P(('grp', 'fs'), 'sp', 'tp'), parts along dimension 0
The draws below stay inside these ranges and needn't reach their ends.
There are 2 independent parts, one for each index of `grp`. The reference program is written for one: setup_inputs(seed, part) draws one part's arguments, and reference() takes and returns one part's arrays. A program takes and returns all parts, laid end to end along the dimension named above; an argument that names none is the same for every part. Nothing has to cross between parts.
All inputs are finite; a program needn't handle non-finite values.
Results may differ from the reference program's by a relative error of at most 0.01.
Values may be sent and summed in bfloat16 or wider, within the bound.
A program may use at most 64 MiB of HBM per device.

```python
import math
import jax
import jax.numpy as jnp
from jax import lax

D = 2048
HEADS = 8
HEAD = 128
CH = 1024
KSIZE = 31
BLOCK = 64
TOK_DEV = 256
LEN = 1024
SEQS = 2
WIDTH_A = 1024
N_TP = 2


def fast_heads(key, fast_count):
    order = jax.random.permutation(jax.random.fold_in(key, 11), HEADS)
    return order < fast_count


def draw_log_decay_rate(key, part):
    fast_key = jax.random.fold_in(key, 12)
    slow_key = jax.random.fold_in(key, 13)
    fast_count = HEADS // 2
    fast_mask = fast_heads(key, fast_count)
    fast_rate = jnp.exp(jax.random.uniform(fast_key, (HEADS,), jnp.float32, math.log(1.0 / 60.0), math.log(1.0 / 30.0))) / 0.7
    slow_rate = 0.5 / (0.7 * LEN) * jnp.exp(jax.random.uniform(slow_key, (HEADS,), jnp.float32, math.log(0.5), 0.0))
    return jnp.log(jnp.where(fast_mask, fast_rate, slow_rate)).astype(jnp.float32)


def draw_write_strength_bias(key, part):
    fast_key = jax.random.fold_in(key, 31)
    slow_key = jax.random.fold_in(key, 32)
    fast_count = HEADS // 2
    fast_mask = fast_heads(key, fast_count)
    fast_level = jax.random.uniform(fast_key, (HEADS,), jnp.float32, -1.0, 1.0)
    slow_level = math.log(0.5 * HEAD / LEN) + jax.random.uniform(slow_key, (HEADS,), jnp.float32, math.log(0.5), 0.0)
    return jnp.where(fast_mask, fast_level, slow_level).astype(jnp.float32)


def draw_decay_spike_added(key, part):
    level_key = jax.random.fold_in(key, 21)
    place_key = jax.random.fold_in(key, 22)
    depth_key = jax.random.fold_in(key, 23)
    blocks = LEN // TOK_DEV
    decay_levels = jax.random.uniform(level_key, (SEQS, blocks, HEADS), jnp.float32, 0.0, 1.0) * (-1.0 / LEN)
    decay_levels = jnp.repeat(decay_levels, TOK_DEV, axis=1)
    places = jax.random.randint(place_key, (SEQS, 2, HEADS), 0, LEN)
    sequence_depths = jnp.log(jax.random.uniform(depth_key, (SEQS, 2, HEADS), jnp.float32, 0.6, 0.8))
    positions = jnp.arange(LEN, dtype=jnp.int32)
    spike_applied = positions[None, :, None, None] == places[:, None, :, :]
    decay_spikes = jnp.sum(jnp.where(spike_applied, sequence_depths[:, None, :, :], 0.0), axis=2)
    return (decay_levels + decay_spikes).astype(jnp.float32)


def draw_convolution_kernel(key, part):
    raw = jnp.clip(jax.random.normal(key, (KSIZE, CH), jnp.float32), -6.0, 6.0)
    channel = jnp.arange(CH, dtype=jnp.float32) / CH
    scales = jnp.exp(math.log(10.0) * channel - 0.5 * math.log(10.0))
    return (raw * KSIZE ** (-0.5) * scales[None, :]).astype(jnp.float32)


def steps_of(stream_key, extent, split, least, largest):
    gain = 1.0
    for dim, shards_of in split:
        steps = jax.random.uniform(jax.random.fold_in(jax.random.fold_in(stream_key, 6), dim), (shards_of,), jnp.float32, least / len(split), largest / len(split))
        gain = gain * jnp.repeat(jnp.exp(steps), extent[dim] // shards_of).reshape((-1,) + (1,) * (len(extent) - 1 - dim))
    return gain


def bell_draw(own_key, dims, width, most, pieces=(), kind=jnp.bfloat16):
    result = width * jax.random.normal(own_key, dims, jnp.float32)
    if pieces:
        result = result * steps_of(own_key, dims, pieces, -0.22, 0.18)
    return jnp.clip(result, -most, most).astype(kind)


def setup_inputs(seed: int = 0, part: int = 0) -> dict:
    splits = jax.random.split(jax.random.key(seed), 19)
    part_keys = jax.random.split(jax.random.fold_in(splits[18], part), 19)
    tokens = bell_draw(part_keys[0], (SEQS, LEN, D), 1.0, 6.0, ((0, 2), (1, 4), (2, 2)))
    input_norm_gain = jnp.clip(1.0 + 0.18 * jax.random.normal(splits[1], (D,), jnp.float32), 0.1, 1.9)
    query_weight = bell_draw(splits[2], (D, WIDTH_A), D ** -0.5, 0.125, ((0, 4), (1, 2)))
    key_weight = bell_draw(splits[3], (D, WIDTH_A), D ** -0.5, 0.125, ((0, 4), (1, 2)))
    value_weight = bell_draw(splits[4], (D, WIDTH_A), D ** -0.5, 0.125, ((0, 4), (1, 2)))
    decay_gate_weight = bell_draw(splits[5], (D, HEADS), D ** -0.5, 0.125)
    write_strength_weight = bell_draw(splits[6], (D, HEADS), D ** -0.5, 0.125)
    up_weight = bell_draw(splits[7], (D, CH), D ** -0.5, 0.125, ((0, 4), (1, 2)))
    gate_half_weight = bell_draw(splits[8], (D, CH), D ** -0.5, 0.125, ((0, 4), (1, 2)))
    log_decay_rate = draw_log_decay_rate(jax.random.fold_in(splits[18], 71), part)
    write_strength_bias = draw_write_strength_bias(jax.random.fold_in(splits[18], 71), part)
    decay_spike_added = draw_decay_spike_added(jax.random.fold_in(jax.random.fold_in(splits[18], part), 71), part)
    starting_state = bell_draw(part_keys[12], (SEQS, HEADS, HEAD, HEAD), 0.5, 4.0, ((0, 2), (1, 2)), jnp.float32)
    head_norm_gain = jnp.clip(1.0 + 0.18 * jax.random.normal(splits[13], (HEAD,), jnp.float32), 0.1, 1.9)
    convolution_kernel = draw_convolution_kernel(jax.random.fold_in(splits[18], 71), part)
    channel_norm_gain = jnp.clip(1.0 + 0.18 * jax.random.normal(splits[15], (CH,), jnp.float32), 0.1, 1.9)
    delta_output_rows = bell_draw(splits[16], (WIDTH_A, D), (WIDTH_A + CH) ** -0.5, 0.125, ((0, 2), (1, 4)))
    convolution_output_rows = bell_draw(splits[17], (CH, D), (WIDTH_A + CH) ** -0.5, 0.125, ((0, 2), (1, 4)))
    return dict(tokens=tokens, input_norm_gain=input_norm_gain, query_weight=query_weight, key_weight=key_weight, value_weight=value_weight, decay_gate_weight=decay_gate_weight, write_strength_weight=write_strength_weight, up_weight=up_weight, gate_half_weight=gate_half_weight, log_decay_rate=log_decay_rate, write_strength_bias=write_strength_bias, decay_spike_added=decay_spike_added, starting_state=starting_state, head_norm_gain=head_norm_gain, convolution_kernel=convolution_kernel, channel_norm_gain=channel_norm_gain, delta_output_rows=delta_output_rows, convolution_output_rows=convolution_output_rows)


EPS = 1e-06
HIGH = lax.Precision.HIGHEST

def unit_rows(values):
    return values * lax.rsqrt(lax.optimization_barrier(jnp.sum(values * values, axis=-1, keepdims=True)) + EPS)

def rounded(values):
    return lax.optimization_barrier(values.astype(jnp.bfloat16)).astype(jnp.float32)

def block_terms(query, keys, values, log_decay, beta):
    rows = keys.shape[0]
    count = rows // BLOCK

    def split_blocks(array):
        return jnp.swapaxes(array.reshape((count, BLOCK) + array.shape[1:]), 1, 2)
    q_blocks, k_blocks, v_blocks = (split_blocks(query), split_blocks(keys), split_blocks(values))
    g_blocks, b_blocks = (split_blocks(log_decay), split_blocks(beta))
    cumdec = jnp.cumsum(g_blocks, axis=-1)
    lower = jnp.tril(jnp.ones((BLOCK, BLOCK), bool))
    strict = jnp.tril(jnp.ones((BLOCK, BLOCK), bool), -1)
    diff = cumdec[..., :, None] - cumdec[..., None, :]
    gamma = jnp.where(lower, jnp.exp(jnp.where(lower, diff, 0.0)), 0.0)
    k_beta = k_blocks * b_blocks[..., None]
    a_matrix = jnp.where(strict, jnp.einsum('nhid,nhjd->nhij', k_beta, k_blocks, precision=HIGH) * gamma, 0.0)
    left_side = a_matrix + jnp.eye(BLOCK, dtype=jnp.float32)
    right_side = jnp.concatenate([v_blocks * b_blocks[..., None], k_beta * jnp.exp(cumdec)[..., None]], axis=-1)
    solved = jax.scipy.linalg.solve_triangular(left_side, right_side, lower=True, unit_diagonal=True)
    width_v = v_blocks.shape[-1]
    updates, w_rows = (solved[..., :width_v], solved[..., width_v:])
    q_k = jnp.where(lower, jnp.einsum('nhid,nhjd->nhij', q_blocks, k_blocks, precision=HIGH) * gamma, 0.0)
    last = cumdec[..., -1]
    k_decayed = k_blocks * jnp.exp(last[..., None] - cumdec)[..., None]
    q_decayed = q_blocks * jnp.exp(cumdec)[..., None]
    return (q_decayed, k_decayed, updates, w_rows, q_k, last)

def block_outputs(start_state, terms):

    def advance(state, input_rows):
        q_decayed, k_decayed, updates, w_rows, q_k, last = input_rows
        v_new = updates - jnp.einsum('hcd,hde->hce', w_rows, state, precision=HIGH)
        output = jnp.einsum('hcd,hde->hce', q_decayed, state, precision=HIGH) + jnp.einsum('hij,hje->hie', q_k, v_new, precision=HIGH)
        state = state * jnp.exp(last)[..., None, None] + jnp.einsum('hcd,hce->hde', k_decayed, v_new, precision=HIGH)
        return (state, output)
    _, outputs = lax.scan(advance, start_state, terms)
    count, heads, blen, width_v = outputs.shape
    return jnp.swapaxes(outputs, 1, 2).reshape(count * blen, heads, width_v)

def single_sequence(tokens, decay_spike_added, starting_state, input_norm_gain, query_weight, key_weight, value_weight, decay_gate_weight, write_strength_weight, up_weight, gate_half_weight, log_decay_rate, write_strength_bias, head_norm_gain, convolution_kernel, channel_norm_gain, delta_output_rows, convolution_output_rows):
    rows = tokens.shape[0]
    token_f = tokens.astype(jnp.float32)
    normed = (token_f * lax.rsqrt(lax.optimization_barrier(jnp.mean(token_f * token_f, axis=-1, keepdims=True)) + EPS) * input_norm_gain).astype(jnp.bfloat16)

    def project_input(weight):
        return rounded(jnp.dot(normed.astype(jnp.float32), weight.astype(jnp.float32), preferred_element_type=jnp.float32))
    shape = (rows, HEADS, HEAD)
    query = unit_rows(jax.nn.silu(project_input(query_weight)).reshape(shape)) * HEAD ** (-0.5)
    keys = unit_rows(jax.nn.silu(project_input(key_weight)).reshape(shape))
    values = jax.nn.silu(project_input(value_weight)).reshape(shape)
    log_decay = -jnp.exp(log_decay_rate) * jax.nn.softplus(project_input(decay_gate_weight)) + decay_spike_added
    beta = jax.nn.sigmoid(project_input(write_strength_weight) + write_strength_bias)
    terms = block_terms(query, keys, values, log_decay, beta)
    attn = block_outputs(starting_state, terms)
    attn_out = (attn * lax.rsqrt(lax.optimization_barrier(jnp.mean(attn * attn, axis=-1, keepdims=True)) + EPS) * head_norm_gain).astype(jnp.bfloat16)
    attn_out = attn_out.reshape(rows, HEADS * HEAD)
    glu = lax.optimization_barrier((project_input(up_weight) * jax.nn.sigmoid(project_input(gate_half_weight))).astype(jnp.bfloat16))
    padded = jnp.concatenate([jnp.zeros((KSIZE - 1, CH), jnp.float32), glu.astype(jnp.float32)], axis=0)
    conv = jnp.zeros((rows, CH), jnp.float32)
    for tap in range(KSIZE):
        conv = conv + convolution_kernel[tap] * padded[tap:tap + rows]
    mean_c = lax.optimization_barrier(jnp.mean(conv, axis=-1, keepdims=True))
    var_c = lax.optimization_barrier(jnp.mean(conv * conv, axis=-1, keepdims=True)) - mean_c * mean_c
    conv_out = jax.nn.silu((conv - mean_c) * lax.rsqrt(var_c + EPS) * channel_norm_gain).astype(jnp.bfloat16)
    attn_group = HEADS * HEAD // N_TP
    conv_group = CH // N_TP
    total = jnp.zeros((rows, D), jnp.float32)
    for group in range(N_TP):
        partial_value = jnp.dot(attn_out[:, group * attn_group:(group + 1) * attn_group].astype(jnp.float32), delta_output_rows[group * attn_group:(group + 1) * attn_group].astype(jnp.float32), preferred_element_type=jnp.float32)
        partial_value = partial_value + jnp.dot(conv_out[:, group * conv_group:(group + 1) * conv_group].astype(jnp.float32), convolution_output_rows[group * conv_group:(group + 1) * conv_group].astype(jnp.float32), preferred_element_type=jnp.float32)
        total = total + rounded(partial_value)
    return total.astype(jnp.bfloat16)

def reference(tokens, input_norm_gain, query_weight, key_weight, value_weight, decay_gate_weight, write_strength_weight, up_weight, gate_half_weight, log_decay_rate, write_strength_bias, decay_spike_added, starting_state, head_norm_gain, convolution_kernel, channel_norm_gain, delta_output_rows, convolution_output_rows):

    def sequence_wise(input_rows):
        sequence_token, sequence_spike, sequence_state = input_rows
        return single_sequence(sequence_token, sequence_spike, sequence_state, input_norm_gain, query_weight, key_weight, value_weight, decay_gate_weight, write_strength_weight, up_weight, gate_half_weight, log_decay_rate, write_strength_bias, head_norm_gain, convolution_kernel, channel_norm_gain, delta_output_rows, convolution_output_rows)
    return lax.map(sequence_wise, (tokens, decay_spike_added, starting_state))
```

```python
import functools

import jax
import jax.numpy as jnp
from jax import lax
from jax.experimental import pallas as pl
from jax.experimental.pallas import tpu as pltpu
from jax.sharding import PartitionSpec as P

HEAD = 128
EPS = 1e-06
HIGH = lax.Precision.HIGHEST


def from_behind(block, axis, distance):
    devices = range(lax.axis_size(axis))
    route = [(i - distance, i) for i in devices if i - distance in devices]
    return lax.ppermute(block, axis, route)


def rounded(values):
    return lax.optimization_barrier(values.astype(jnp.bfloat16)).astype(jnp.float32)


def mm(a, b, precision=None):
    return jnp.dot(a, b, preferred_element_type=jnp.float32, precision=precision)


def mm_nt(a, b, precision=None):
    return lax.dot_general(
        a, b, (((1,), (1,)), ((), ())), preferred_element_type=jnp.float32, precision=precision
    )


def mm_tn(a, b, precision=None):
    return lax.dot_general(
        a, b, (((0,), (0,)), ((), ())), preferred_element_type=jnp.float32, precision=precision
    )


def silu(x):
    return x * jax.nn.sigmoid(x)


def unit(x):
    return x * lax.rsqrt(jnp.sum(x * x, axis=-1, keepdims=True) + EPS)


def delta_kernel(q_ref, k_ref, v_ref, cum_col_ref, cum_row_ref, beta_ref, p_ref, u_ref, m_ref, o_ref):
    units, rows, width = q_ref.shape
    row_id = lax.broadcasted_iota(jnp.int32, (rows, rows), 0)
    col_id = lax.broadcasted_iota(jnp.int32, (rows, rows), 1)
    lower = row_id >= col_id
    strict = row_id > col_id
    eye = jnp.where(row_id == col_id, 1.0, 0.0)
    here = range(units)
    query = [unit(silu(q_ref[u].astype(jnp.float32))) * HEAD ** (-0.5) for u in here]
    keys = [unit(silu(k_ref[u].astype(jnp.float32))) for u in here]
    values = [silu(v_ref[u].astype(jnp.float32)) for u in here]
    gamma = [
        jnp.where(lower, jnp.exp(jnp.where(lower, cum_col_ref[u] - cum_row_ref[u], 0.0)), 0.0)
        for u in here
    ]
    k_beta = [keys[u] * beta_ref[u] for u in here]
    a = [jnp.where(strict, mm_nt(k_beta[u], keys[u], HIGH) * gamma[u], 0.0) for u in here]
    size = 1
    t = None
    while size < rows:
        pair = 2 * size
        off = (row_id // pair == col_id // pair) & (row_id % pair >= size) & (col_id % pair < size)
        part = [jnp.where(off, a[u], 0.0) for u in here]
        if t is None:
            t = [eye - part[u] for u in here]
        else:
            half = [mm(part[u], t[u], HIGH) for u in here]
            t = [t[u] - mm(t[u], half[u], HIGH) for u in here]
        size = pair
    for u in here:
        grow = jnp.exp(cum_col_ref[u])
        last = cum_col_ref[u][rows - 1 :, :]
        right = jnp.concatenate([values[u] * beta_ref[u], k_beta[u] * grow], axis=1)
        solved = mm(t[u], right, HIGH)
        q_k = mm_nt(query[u], keys[u]) * gamma[u]
        k_decayed = keys[u] * jnp.exp(last - cum_col_ref[u])
        inner = mm(q_k, solved)
        p_ref[u] = query[u] * grow - inner[:, width:]
        u_ref[u] = inner[:, :width]
        state = mm_tn(k_decayed, solved, HIGH)
        m_ref[u] = eye[:width, :width] * jnp.exp(last) - state[:, width:]
        o_ref[u] = state[:, :width]


def delta_terms(query, keys, values, cum, beta):
    units, rows, width = query.shape
    f32 = jnp.float32
    group = next(g for g in (4, 2, 1) if units % g == 0)

    def spec(*dims):
        return pl.BlockSpec((group,) + dims, lambda i: (i, 0, 0))

    return pl.pallas_call(
        delta_kernel,
        grid=(units // group,),
        out_shape=(
            jax.ShapeDtypeStruct((units, rows, width), f32),
            jax.ShapeDtypeStruct((units, rows, width), f32),
            jax.ShapeDtypeStruct((units, width, width), f32),
            jax.ShapeDtypeStruct((units, width, width), f32),
        ),
        in_specs=[spec(rows, width)] * 3 + [spec(rows, 1), spec(1, rows), spec(rows, 1)],
        out_specs=(spec(rows, width), spec(rows, width), spec(width, width), spec(width, width)),
        compiler_params=pltpu.CompilerParams(vmem_limit_bytes=48 * 1024 * 1024),
        cost_estimate=pl.CostEstimate(
            flops=units * rows * rows * rows * 180, bytes_accessed=units * rows * width * 16, transcendentals=0
        ),
    )(query, keys, values, cum[..., None], cum[:, None, :], beta[..., None])


def on_device(
    cols,
    tokens,
    input_norm_gain,
    query_weight,
    key_weight,
    value_weight,
    decay_gate_weight,
    write_strength_weight,
    up_weight,
    gate_half_weight,
    log_decay_rate,
    write_strength_bias,
    decay_spike_added,
    starting_state,
    head_norm_gain,
    convolution_kernel,
    channel_norm_gain,
    delta_output_rows,
    convolution_output_rows,
):
    rows = tokens.shape[1]
    count = 1
    for axis in cols:
        count *= lax.axis_size(axis)
    channels = convolution_kernel.shape[1]
    taps = convolution_kernel.shape[0]
    tp_index = lax.axis_index("tp")
    sp_index = lax.axis_index("sp")
    col = lax.axis_index(cols) if cols else 0
    heads_tp = query_weight.shape[1] // HEAD
    heads = heads_tp // count
    chan_tp = up_weight.shape[1]
    chan = chan_tp // count
    head_start = tp_index * heads_tp + col * heads
    chan_start = tp_index * chan_tp + col * chan

    def mine(weight, axis, width):
        return lax.dynamic_slice_in_dim(weight, col * width, width, axis)

    wide = heads * HEAD
    stacked = jnp.concatenate(
        [mine(w, 1, wide) for w in (query_weight, key_weight, value_weight)]
        + [mine(w, 1, chan) for w in (up_weight, gate_half_weight)],
        axis=1,
    )
    gathered_in = lax.all_gather(stacked, "sp", axis=0, tiled=True)
    token_all = lax.all_gather(tokens[0], cols + ("tp",), axis=0, tiled=False)
    token_all = token_all.reshape((count, -1, rows, tokens.shape[2]))
    token_all = jnp.swapaxes(token_all, 1, 2).reshape((count * rows, -1))
    out_rows = jnp.concatenate(
        [mine(delta_output_rows, 0, wide), mine(convolution_output_rows, 0, chan)], axis=0
    )
    spikes = decay_spike_added[0]
    start_state = starting_state[0]
    if cols:
        spikes = lax.all_gather(spikes, cols, axis=0, tiled=False)
        start_state = lax.all_to_all(
            start_state.reshape((count, heads, HEAD, HEAD)), cols, 0, 0, tiled=False
        ).reshape((count * heads, HEAD, HEAD))
    spikes = spikes.reshape((count, rows, heads_tp))
    spikes = lax.dynamic_slice_in_dim(spikes, col * heads, heads, 2)

    token_f = token_all.astype(jnp.float32)
    normed = (
        token_f
        * lax.rsqrt(jnp.mean(token_f * token_f, axis=-1, keepdims=True) + EPS)
        * input_norm_gain
    ).astype(jnp.bfloat16)

    gate_cols = jnp.concatenate(
        [
            lax.dynamic_slice_in_dim(decay_gate_weight, head_start, heads, 1),
            lax.dynamic_slice_in_dim(write_strength_weight, head_start, heads, 1),
        ],
        axis=1,
    )
    small = rounded(jnp.dot(normed, gate_cols, preferred_element_type=jnp.float32))
    small = small.reshape((count, rows, 2 * heads))
    rates = jnp.exp(lax.dynamic_slice_in_dim(log_decay_rate, head_start, heads, 0))
    bias = lax.dynamic_slice_in_dim(write_strength_bias, head_start, heads, 0)
    log_decay = -rates * jax.nn.softplus(small[..., :heads]) + spikes
    beta = jax.nn.sigmoid(small[..., heads:] + bias)
    ones = jnp.tril(jnp.ones((rows, rows), jnp.float32))
    cum = jnp.einsum("ij,cjh->chi", ones, log_decay, precision=HIGH).reshape((count * heads, rows))
    beta = jnp.swapaxes(beta, 1, 2).reshape((count * heads, rows))

    raw = jnp.dot(normed, gathered_in, preferred_element_type=jnp.float32).astype(jnp.bfloat16)

    def heads_of(block):
        block = block.reshape((count, rows, heads, HEAD))
        return jnp.swapaxes(block, 1, 2).reshape((count * heads, rows, HEAD))

    p_rows, u_rows, maps, offsets = delta_terms(
        heads_of(raw[:, :wide]),
        heads_of(raw[:, wide : 2 * wide]),
        heads_of(raw[:, 2 * wide : 3 * wide]),
        cum,
        beta,
    )
    up = raw[:, 3 * wide : 3 * wide + chan].astype(jnp.float32)
    gate = raw[:, 3 * wide + chan :].astype(jnp.float32)
    glu = (up * jax.nn.sigmoid(gate)).astype(jnp.bfloat16).reshape((count, rows, chan))
    rim = from_behind(glu[:, rows - (taps - 1) :], "sp", 1)
    first = sp_index == 0
    state = jnp.where(first, start_state, jnp.zeros_like(start_state))
    for _ in range(lax.axis_size("sp") - 1):
        sent = jnp.einsum("hde,hef->hdf", maps, state, precision=HIGH) + offsets
        state = jnp.where(first, start_state, from_behind(sent, "sp", 1))

    extended = jnp.concatenate([rim, glu], axis=1).astype(jnp.float32)
    taps_here = lax.dynamic_slice_in_dim(convolution_kernel, chan_start, chan, 1)
    conv = jnp.zeros((count, rows, chan), jnp.float32)
    for tap in range(taps):
        conv = conv + taps_here[tap] * extended[:, tap : tap + rows]
    sums = jnp.stack([jnp.sum(conv, axis=-1), jnp.sum(conv * conv, axis=-1)])
    sums = lax.psum(sums, cols + ("tp",))
    mean_c = (sums[0] / channels)[..., None]
    var_c = (sums[1] / channels)[..., None] - mean_c * mean_c
    gain = lax.dynamic_slice_in_dim(channel_norm_gain, chan_start, chan, 0)
    conv_out = jax.nn.silu((conv - mean_c) * lax.rsqrt(var_c + EPS) * gain).astype(jnp.bfloat16)

    attn = jnp.einsum("hcd,hde->hce", p_rows, state) + u_rows
    attn_out = (
        attn * lax.rsqrt(jnp.mean(attn * attn, axis=-1, keepdims=True) + EPS) * head_norm_gain
    ).astype(jnp.bfloat16)
    attn_out = jnp.swapaxes(attn_out.reshape((count, heads, rows, HEAD)), 1, 2)
    attn_out = attn_out.reshape((count * rows, wide))
    mixer = jnp.concatenate([attn_out, conv_out.reshape((count * rows, chan))], axis=1)
    gathered_out = lax.all_gather(out_rows, "sp", axis=1, tiled=True)
    term = jnp.dot(mixer, gathered_out, preferred_element_type=jnp.float32).astype(jnp.bfloat16)
    half = term.shape[1] // lax.axis_size("tp")
    term = jnp.swapaxes(term.reshape((count, rows, -1, half)), 1, 2).reshape((-1, rows, half))
    mixed = lax.psum_scatter(term, cols + ("tp",), scatter_dimension=0, tiled=True)
    return mixed


def split_axes(mesh, heads_tp, chan_tp):
    for axes in (("grp", "fs"), ("fs",), ("grp",)):
        count = 1
        for axis in axes:
            count *= mesh.shape[axis]
        if heads_tp % count == 0 and chan_tp % (count * 128) == 0:
            return axes
    return ()


def solution(mesh):
    def whole(*args):
        heads_tp = args[2].shape[1] // HEAD // mesh.shape["tp"]
        chan_tp = args[7].shape[1] // mesh.shape["tp"]
        cols = split_axes(mesh, heads_tp, chan_tp)
        return jax.shard_map(
            functools.partial(on_device, cols),
            mesh=mesh,
            in_specs=(
                P(("grp", "fs"), "sp", "tp"),
                P(),
                P("sp", "tp"),
                P("sp", "tp"),
                P("sp", "tp"),
                P(),
                P(),
                P("sp", "tp"),
                P("sp", "tp"),
                P(),
                P(),
                P(("grp", "fs"), "sp", "tp"),
                P(("grp", "fs"), "tp", None, None),
                P(),
                P(),
                P(),
                P("tp", "sp"),
                P("tp", "sp"),
            ),
            out_specs=P(("grp", "fs"), "sp", "tp"),
            check_vma=False,
        )(*args)

    return whole
```

```python
import functools

import jax
import jax.numpy as jnp
from jax import lax
from jax.experimental import pallas as pl
from jax.experimental.pallas import tpu as pltpu
from jax.sharding import PartitionSpec as P

HEAD = 128
EPS = 1e-06
HIGH = lax.Precision.HIGHEST


def from_behind(block, axis, distance):
    devices = range(lax.axis_size(axis))
    route = [(i - distance, i) for i in devices if i - distance in devices]
    return lax.ppermute(block, axis, route)


def rounded(values):
    return lax.optimization_barrier(values.astype(jnp.bfloat16)).astype(jnp.float32)


def mm(a, b, precision=None):
    return jnp.dot(a, b, preferred_element_type=jnp.float32, precision=precision)


def mm_nt(a, b, precision=None):
    return lax.dot_general(
        a, b, (((1,), (1,)), ((), ())), preferred_element_type=jnp.float32, precision=precision
    )


def mm_tn(a, b, precision=None):
    return lax.dot_general(
        a, b, (((0,), (0,)), ((), ())), preferred_element_type=jnp.float32, precision=precision
    )


def silu(x):
    return x * jax.nn.sigmoid(x)


def unit(x):
    return x * lax.rsqrt(jnp.sum(x * x, axis=-1, keepdims=True) + EPS)


MESH = pl.DeviceIdType.MESH


def column_peer(cols, sizes, index):
    where = {}
    for axis, size in reversed(list(zip(cols, sizes))):
        where[axis] = lax.rem(index, size)
        index = index // size
    return where


def column_index(cols, sizes):
    index = 0
    for axis, size in zip(cols, sizes):
        index = index * size + lax.axis_index(axis)
    return index


def greet(peers):
    barrier = pltpu.get_barrier_semaphore()
    for peer in peers:
        pl.semaphore_signal(barrier, inc=1, device_id=peer, device_id_type=MESH)
    pl.semaphore_wait(barrier, len(peers))


def send(src, dst, send_sem, recv_sem, peer):
    copy = pltpu.make_async_remote_copy(
        src_ref=src, dst_ref=dst, send_sem=send_sem, recv_sem=recv_sem, device_id=peer, device_id_type=MESH
    )
    copy.start()
    return copy


def gather_kernel(
    cols, sizes, ring, tok_ref, w_ref, spike_ref, state_ref, gain_ref, gates_ref,
    raw_ref, small_ref, spikes_ref, states_ref,
    tok_all, w_all, normed,
    tok_send, tok_recv, fwd_send, fwd_recv, w_send, w_recv, spk_send, spk_recv, st_send, st_recv, local_sem,
):
    rows, half = tok_ref.shape
    depth = w_ref.shape[0]
    count = 1
    for size in sizes:
        count *= size
    col = column_index(cols, sizes)
    tp = lax.axis_index("tp")
    sp = lax.axis_index("sp")
    partner = {"tp": 1 - tp}
    peers = [column_peer(cols, sizes, lax.rem(col + d, count)) for d in range(count)]
    right = {"sp": lax.rem(sp + 1, ring)}
    left = {"sp": lax.rem(sp + ring - 1, ring)}

    def place(source, side):
        return tok_all.at[
            pl.ds(pl.multiple_of(source * rows, rows), rows), pl.ds(pl.multiple_of(side * half, half), half)
        ]

    mid = depth // 2

    def shard(owner, top):
        begin = owner * depth + (0 if top else mid)
        return w_all.at[pl.ds(pl.multiple_of(begin, mid), mid), :]

    own = pltpu.make_async_copy(tok_ref, place(col, tp), local_sem.at[0])
    own.start()
    own_w = pltpu.make_async_copy(
        w_ref, w_all.at[pl.ds(pl.multiple_of(sp * depth, depth), depth), :], local_sem.at[1]
    )
    own_w.start()
    own_spike = pltpu.make_async_copy(spike_ref, spikes_ref.at[col], local_sem.at[2])
    own_spike.start()
    own_state = pltpu.make_async_copy(state_ref.at[col], states_ref.at[col], local_sem.at[3])
    own_state.start()
    greet([right, left, partner] + peers[1:])

    fwd = {0: send(tok_ref, place(col, tp), fwd_send.at[0], fwd_recv.at[0], partner)}
    w_copies = []

    def ring_step(step):
        behind = lax.rem(sp - step + ring, ring)
        ahead = lax.rem(sp + step, ring)
        top = w_ref.at[pl.ds(0, mid), :] if step == 0 else shard(behind, True)
        low = w_ref.at[pl.ds(mid, mid), :] if step == 0 else shard(ahead, False)
        w_copies.append(
            (
                send(top, shard(behind, True), w_send.at[0, step], w_recv.at[0, step], right),
                send(low, shard(ahead, False), w_send.at[1, step], w_recv.at[1, step], left),
            )
        )

    if ring > 1:
        ring_step(0)
    toks, spikes, states = {}, {}, {}
    for d in range(1, count):
        peer = peers[d]
        spikes[d] = send(spike_ref, spikes_ref.at[col], spk_send.at[d], spk_recv.at[d], peer)
        toks[d] = send(tok_ref, place(col, tp), tok_send.at[d], tok_recv.at[d], peer)
    for d in range(1, count):
        target = lax.rem(col + d, count)
        states[d] = send(state_ref.at[target], states_ref.at[col], st_send.at[d], st_recv.at[d], peers[d])

    def normalise(source):
        span = pl.ds(pl.multiple_of(source * rows, rows), rows)
        block = tok_all[span, :].astype(jnp.float32)
        scale = lax.rsqrt(jnp.mean(block * block, axis=-1, keepdims=True) + EPS)
        normed[span, :] = (block * scale * gain_ref[...]).astype(jnp.bfloat16)

    own.wait()
    fwd[0].wait()
    normalise(col)
    for i in range(max(ring - 1, count - 1)):
        if i < ring - 1:
            for copy in w_copies[i]:
                copy.wait()
            if i + 1 < ring - 1:
                ring_step(i + 1)
        d = i + 1
        if d < count:
            toks[d].wait()
            source = lax.rem(col - d + count, count)
            fwd[d] = send(place(source, tp), place(source, tp), fwd_send.at[d], fwd_recv.at[d], partner)
            if d > 1:
                fwd[d - 1].wait()
                normalise(lax.rem(col - d + 1 + count, count))
    if count > 1:
        fwd[count - 1].wait()
        normalise(lax.rem(col + 1, count))
    own_w.wait()
    own_spike.wait()
    own_state.wait()
    for d in range(1, count):
        spikes[d].wait()
        states[d].wait()

    @pl.loop(0, count)
    def _(c):
        span = pl.ds(pl.multiple_of(c * rows, rows), rows)
        block = normed[span, :]
        raw_ref[span, :] = mm(block, w_all[...]).astype(jnp.bfloat16)
        small_ref[span, :] = mm(block, gates_ref[...])


def gather_project(cols, sizes, ring, tokens, weights, spikes, states, gain, gates):
    rows, half = tokens.shape
    depth, width = weights.shape
    count = states.shape[0]
    total = depth * ring
    dma = pltpu.SemaphoreType.DMA
    vmem = pl.BlockSpec(memory_space=pltpu.VMEM)
    anywhere = pl.BlockSpec(memory_space=pl.ANY)
    return pl.pallas_call(
        functools.partial(gather_kernel, cols, sizes, ring),
        out_shape=(
            jax.ShapeDtypeStruct((count * rows, width), jnp.bfloat16),
            jax.ShapeDtypeStruct((count * rows, gates.shape[1]), jnp.float32),
            jax.ShapeDtypeStruct((count,) + spikes.shape, jnp.float32),
            jax.ShapeDtypeStruct(states.shape, jnp.float32),
        ),
        in_specs=[anywhere, anywhere, vmem, vmem, vmem, vmem],
        out_specs=(vmem,) * 4,
        scratch_shapes=[
            pltpu.VMEM((count * rows, total), jnp.bfloat16),
            pltpu.VMEM((total, width), jnp.bfloat16),
            pltpu.VMEM((count * rows, total), jnp.bfloat16),
            dma((count,)), dma((count,)), dma((count,)), dma((count,)),
            dma((2, ring)), dma((2, ring)),
            dma((count,)), dma((count,)), dma((count,)), dma((count,)),
            dma((4,)),
        ],
        compiler_params=pltpu.CompilerParams(
            collective_id=1, has_side_effects=True, vmem_limit_bytes=48 * 1024 * 1024
        ),
        name="gather_project",
    )(tokens, weights, spikes, states, gain, gates)


def sum_kernel(cols, sizes, x_ref, o_ref, slots, send_sem, recv_sem):
    count = slots.shape[0]
    names, widths = cols + ("tp",), sizes + (2,)
    me = column_index(names, widths)
    peers = [column_peer(names, widths, lax.rem(me + d, count)) for d in range(count)]
    greet(peers[1:])
    copies = [
        send(x_ref, slots.at[d], send_sem.at[d], recv_sem.at[d], peers[d]) for d in range(1, count)
    ]
    total = x_ref[...]
    for d in range(1, count):
        copies[d - 1].wait()
        total = total + slots[d]
    o_ref[...] = total


def sum_small(cols, sizes, x):
    count = 2
    for size in sizes:
        count *= size
    return pl.pallas_call(
        functools.partial(sum_kernel, cols, sizes),
        out_shape=jax.ShapeDtypeStruct(x.shape, x.dtype),
        in_specs=[pl.BlockSpec(memory_space=pltpu.VMEM)],
        out_specs=pl.BlockSpec(memory_space=pltpu.VMEM),
        scratch_shapes=[
            pltpu.VMEM((count,) + x.shape, x.dtype),
            pltpu.SemaphoreType.DMA((count,)),
            pltpu.SemaphoreType.DMA((count,)),
        ],
        compiler_params=pltpu.CompilerParams(collective_id=2, has_side_effects=True),
        name="sum_small",
    )(x)


def project_kernel(
    cols, sizes, mix_ref, w_ref, out_ref, to_pair, from_pair, to_col, from_col,
    pair_send, pair_recv, col_send, col_recv,
):
    count, rows, half = from_col.shape
    col = column_index(cols, sizes)
    tp = lax.axis_index("tp")
    partner = {"tp": 1 - tp}
    peers = [column_peer(cols, sizes, lax.rem(col + d, count)) for d in range(count)]
    greet([partner] + peers[1:])
    order = [d for d in range(1, count)] + [0]

    def part(d, side):
        target = lax.rem(col + d, count)
        block = mix_ref[pl.ds(pl.multiple_of(target * rows, rows), rows), :]
        return mm(block, w_ref[:, pl.ds(pl.multiple_of(side * half, half), half)])

    pairs, sends = {}, {}

    def to_partner(d):
        to_pair[d] = part(d, 1 - tp).astype(jnp.bfloat16)
        pairs[d] = send(to_pair.at[d], from_pair.at[d], pair_send.at[d], pair_recv.at[d], partner)

    to_partner(order[0])
    for i, d in enumerate(order):
        if i + 1 < count:
            to_partner(order[i + 1])
        mine = part(d, tp)
        pairs[d].wait()
        mine = mine + from_pair[d].astype(jnp.float32)
        if d:
            to_col[d] = mine.astype(jnp.bfloat16)
            sends[d] = send(to_col.at[d], from_col.at[d], col_send.at[d], col_recv.at[d], peers[d])
    total = mine
    for d in range(1, count):
        sends[d].wait()
        total = total + from_col[d].astype(jnp.float32)
    out_ref[...] = total.astype(jnp.bfloat16)


def project_out(cols, sizes, rows, mixer, weights):
    count = mixer.shape[0] // rows
    half = weights.shape[1] // 2
    bf16 = jnp.bfloat16
    dma = pltpu.SemaphoreType.DMA
    return pl.pallas_call(
        functools.partial(project_kernel, cols, sizes),
        out_shape=jax.ShapeDtypeStruct((rows, half), bf16),
        in_specs=[pl.BlockSpec(memory_space=pltpu.VMEM)] * 2,
        out_specs=pl.BlockSpec(memory_space=pltpu.VMEM),
        scratch_shapes=[pltpu.VMEM((count, rows, half), bf16)] * 4 + [dma((count,))] * 4,
        compiler_params=pltpu.CompilerParams(
            collective_id=3, has_side_effects=True, vmem_limit_bytes=48 * 1024 * 1024
        ),
        name="project_out",
    )(mixer, weights)


def delta_kernel(q_ref, k_ref, v_ref, cum_col_ref, cum_row_ref, beta_ref, p_ref, u_ref, m_ref, o_ref):
    units, rows, width = q_ref.shape
    row_id = lax.broadcasted_iota(jnp.int32, (rows, rows), 0)
    col_id = lax.broadcasted_iota(jnp.int32, (rows, rows), 1)
    lower = row_id >= col_id
    strict = row_id > col_id
    eye = jnp.where(row_id == col_id, 1.0, 0.0)
    here = range(units)
    query = [unit(silu(q_ref[u].astype(jnp.float32))) * HEAD ** (-0.5) for u in here]
    keys = [unit(silu(k_ref[u].astype(jnp.float32))) for u in here]
    values = [silu(v_ref[u].astype(jnp.float32)) for u in here]
    gamma = [
        jnp.where(lower, jnp.exp(jnp.where(lower, cum_col_ref[u] - cum_row_ref[u], 0.0)), 0.0)
        for u in here
    ]
    k_beta = [keys[u] * beta_ref[u] for u in here]
    a = [jnp.where(strict, mm_nt(k_beta[u], keys[u], HIGH) * gamma[u], 0.0) for u in here]
    size = 1
    t = None
    while size < rows:
        pair = 2 * size
        off = (row_id // pair == col_id // pair) & (row_id % pair >= size) & (col_id % pair < size)
        part = [jnp.where(off, a[u], 0.0) for u in here]
        if t is None:
            t = [eye - part[u] for u in here]
        else:
            half = [mm(part[u], t[u], HIGH) for u in here]
            t = [t[u] - mm(t[u], half[u], HIGH) for u in here]
        size = pair
    for u in here:
        grow = jnp.exp(cum_col_ref[u])
        last = cum_col_ref[u][rows - 1 :, :]
        right = jnp.concatenate([values[u] * beta_ref[u], k_beta[u] * grow], axis=1)
        solved = mm(t[u], right, HIGH)
        q_k = mm_nt(query[u], keys[u]) * gamma[u]
        k_decayed = keys[u] * jnp.exp(last - cum_col_ref[u])
        inner = mm(q_k, solved)
        p_ref[u] = query[u] * grow - inner[:, width:]
        u_ref[u] = inner[:, :width]
        state = mm_tn(k_decayed, solved, HIGH)
        m_ref[u] = eye[:width, :width] * jnp.exp(last) - state[:, width:]
        o_ref[u] = state[:, :width]


def delta_terms(query, keys, values, cum, beta):
    units, rows, width = query.shape
    f32 = jnp.float32
    group = next(g for g in (4, 2, 1) if units % g == 0)

    def spec(*dims):
        return pl.BlockSpec((group,) + dims, lambda i: (i, 0, 0))

    return pl.pallas_call(
        delta_kernel,
        grid=(units // group,),
        out_shape=(
            jax.ShapeDtypeStruct((units, rows, width), f32),
            jax.ShapeDtypeStruct((units, rows, width), f32),
            jax.ShapeDtypeStruct((units, width, width), f32),
            jax.ShapeDtypeStruct((units, width, width), f32),
        ),
        in_specs=[spec(rows, width)] * 3 + [spec(rows, 1), spec(1, rows), spec(rows, 1)],
        out_specs=(spec(rows, width), spec(rows, width), spec(width, width), spec(width, width)),
        compiler_params=pltpu.CompilerParams(vmem_limit_bytes=48 * 1024 * 1024),
        cost_estimate=pl.CostEstimate(
            flops=units * rows * rows * rows * 180, bytes_accessed=units * rows * width * 16, transcendentals=0
        ),
    )(query, keys, values, cum[..., None], cum[:, None, :], beta[..., None])


def on_device(
    cols,
    tokens,
    input_norm_gain,
    query_weight,
    key_weight,
    value_weight,
    decay_gate_weight,
    write_strength_weight,
    up_weight,
    gate_half_weight,
    log_decay_rate,
    write_strength_bias,
    decay_spike_added,
    starting_state,
    head_norm_gain,
    convolution_kernel,
    channel_norm_gain,
    delta_output_rows,
    convolution_output_rows,
):
    rows = tokens.shape[1]
    count = 1
    for axis in cols:
        count *= lax.axis_size(axis)
    channels = convolution_kernel.shape[1]
    taps = convolution_kernel.shape[0]
    tp_index = lax.axis_index("tp")
    sp_index = lax.axis_index("sp")
    col = lax.axis_index(cols) if cols else 0
    heads_tp = query_weight.shape[1] // HEAD
    heads = heads_tp // count
    chan_tp = up_weight.shape[1]
    chan = chan_tp // count
    head_start = tp_index * heads_tp + col * heads
    chan_start = tp_index * chan_tp + col * chan

    def mine(weight, axis, width):
        return lax.dynamic_slice_in_dim(weight, col * width, width, axis)

    wide = heads * HEAD
    stacked = jnp.concatenate(
        [mine(w, 1, wide) for w in (query_weight, key_weight, value_weight)]
        + [mine(w, 1, chan) for w in (up_weight, gate_half_weight)],
        axis=1,
    )
    out_rows = jnp.concatenate(
        [mine(delta_output_rows, 0, wide), mine(convolution_output_rows, 0, chan)], axis=0
    )
    sizes = tuple(lax.axis_size(axis) for axis in cols)
    gate_cols = jnp.concatenate(
        [
            lax.dynamic_slice_in_dim(decay_gate_weight, head_start, heads, 1),
            lax.dynamic_slice_in_dim(write_strength_weight, head_start, heads, 1),
        ],
        axis=1,
    )
    gate_cols = jnp.pad(gate_cols, ((0, 0), (0, 128 - 2 * heads)))
    raw, small, spikes, start_state = gather_project(
        cols,
        sizes,
        lax.axis_size("sp"),
        tokens[0],
        stacked,
        decay_spike_added[0].T.reshape((-1, 128)),
        starting_state[0].reshape((count, heads * HEAD, HEAD)),
        input_norm_gain[None],
        gate_cols,
    )
    start_state = start_state.reshape((count * heads, HEAD, HEAD))
    spikes = spikes.reshape((count, heads_tp, rows))
    spikes = jnp.swapaxes(lax.dynamic_slice_in_dim(spikes, col * heads, heads, 1), 1, 2)
    small = rounded(small[:, : 2 * heads]).reshape((count, rows, 2 * heads))
    rates = jnp.exp(lax.dynamic_slice_in_dim(log_decay_rate, head_start, heads, 0))
    bias = lax.dynamic_slice_in_dim(write_strength_bias, head_start, heads, 0)
    log_decay = -rates * jax.nn.softplus(small[..., :heads]) + spikes
    beta = jax.nn.sigmoid(small[..., heads:] + bias)
    ones = jnp.tril(jnp.ones((rows, rows), jnp.float32))
    cum = jnp.einsum("ij,cjh->chi", ones, log_decay, precision=HIGH).reshape((count * heads, rows))
    beta = jnp.swapaxes(beta, 1, 2).reshape((count * heads, rows))

    def heads_of(block):
        block = block.reshape((count, rows, heads, HEAD))
        return jnp.swapaxes(block, 1, 2).reshape((count * heads, rows, HEAD))

    p_rows, u_rows, maps, offsets = delta_terms(
        heads_of(raw[:, :wide]),
        heads_of(raw[:, wide : 2 * wide]),
        heads_of(raw[:, 2 * wide : 3 * wide]),
        cum,
        beta,
    )
    up = raw[:, 3 * wide : 3 * wide + chan].astype(jnp.float32)
    gate = raw[:, 3 * wide + chan :].astype(jnp.float32)
    glu = (up * jax.nn.sigmoid(gate)).astype(jnp.bfloat16).reshape((count, rows, chan))
    rim = from_behind(glu[:, rows - (taps - 1) :], "sp", 1)
    first = sp_index == 0
    state = jnp.where(first, start_state, jnp.zeros_like(start_state))
    for _ in range(lax.axis_size("sp") - 1):
        sent = jnp.einsum("hde,hef->hdf", maps, state, precision=HIGH) + offsets
        state = jnp.where(first, start_state, from_behind(sent, "sp", 1))

    extended = jnp.concatenate([rim, glu], axis=1).astype(jnp.float32)
    taps_here = lax.dynamic_slice_in_dim(convolution_kernel, chan_start, chan, 1)
    conv = jnp.zeros((count, rows, chan), jnp.float32)
    for tap in range(taps):
        conv = conv + taps_here[tap] * extended[:, tap : tap + rows]
    sums = jnp.stack([jnp.sum(conv, axis=-1), jnp.sum(conv * conv, axis=-1)])
    sums = sum_small(cols, sizes, sums.reshape((-1, 128))).reshape(sums.shape)
    mean_c = (sums[0] / channels)[..., None]
    var_c = (sums[1] / channels)[..., None] - mean_c * mean_c
    gain = lax.dynamic_slice_in_dim(channel_norm_gain, chan_start, chan, 0)
    conv_out = jax.nn.silu((conv - mean_c) * lax.rsqrt(var_c + EPS) * gain).astype(jnp.bfloat16)

    attn = jnp.einsum("hcd,hde->hce", p_rows, state) + u_rows
    attn_out = (
        attn * lax.rsqrt(jnp.mean(attn * attn, axis=-1, keepdims=True) + EPS) * head_norm_gain
    ).astype(jnp.bfloat16)
    attn_out = jnp.swapaxes(attn_out.reshape((count, heads, rows, HEAD)), 1, 2)
    attn_out = attn_out.reshape((count * rows, wide))
    mixer = jnp.concatenate([attn_out, conv_out.reshape((count * rows, chan))], axis=1)
    gathered_out = lax.all_gather(out_rows, "sp", axis=1, tiled=True)
    return project_out(cols, sizes, rows, mixer, gathered_out)[None]


def split_axes(mesh, heads_tp, chan_tp):
    for axes in (("grp", "fs"), ("fs",), ("grp",)):
        count = 1
        for axis in axes:
            count *= mesh.shape[axis]
        if heads_tp % count == 0 and chan_tp % (count * 128) == 0:
            return axes
    return ()


def solution(mesh):
    def whole(*args):
        heads_tp = args[2].shape[1] // HEAD // mesh.shape["tp"]
        chan_tp = args[7].shape[1] // mesh.shape["tp"]
        cols = split_axes(mesh, heads_tp, chan_tp)
        return jax.shard_map(
            functools.partial(on_device, cols),
            mesh=mesh,
            in_specs=(
                P(("grp", "fs"), "sp", "tp"),
                P(),
                P("sp", "tp"),
                P("sp", "tp"),
                P("sp", "tp"),
                P(),
                P(),
                P("sp", "tp"),
                P("sp", "tp"),
                P(),
                P(),
                P(("grp", "fs"), "sp", "tp"),
                P(("grp", "fs"), "tp", None, None),
                P(),
                P(),
                P(),
                P("tp", "sp"),
                P("tp", "sp"),
            ),
            out_specs=P(("grp", "fs"), "sp", "tp"),
            check_vma=False,
        )(*args)

    return whole
```
